32 devices in a mesh: ep: 8 (over z, x), tp: 4 (over y, core).
Axes of the slice: x: 2, y: 2, z: 4, core: 2. Of those that a mesh axis runs over, the one named last changes fastest.
Arguments:
- mixer_input: bfloat16 [4096, 2048], P('ep'), may hold values from -5.5 to 5.5
- expert_input: bfloat16 [4096, 2048], P('ep'), may hold values from -6 to 6
- gain_mixer: float32 [2048], replicated, may hold values from 0.1 to 1.9
- gain_expert: float32 [2048], replicated, may hold values from 0.1 to 1.9
- query_weight: bfloat16 [2048, 1536], P(None, 'tp')
- key_weight: bfloat16 [2048, 256], P(None, 'tp')
- value_weight: bfloat16 [2048, 256], P(None, 'tp'), may hold values from -0.125 to 0.125
- sink_logits: float32 [24], P('tp'), may hold values from 2 to 6
- output_weight: bfloat16 [1536, 2048], P('tp'), may hold values from -0.75 to 0.75
- expert_choice: int32 [4096, 2], P('ep'), may hold values from 0 to 7, all different within a row; in each aligned block of 128 rows (0 to 127, 128 to 255, ...) at most 64 rows name the same one
- route_weights: float32 [4096, 2], P('ep'), may hold values from 0.2 to 1.2
- expert_gate: bfloat16 [8, 2048, 1024], P('ep', None, 'tp'), may hold values from -0.125 to 0.125
- expert_up: bfloat16 [8, 2048, 1024], P('ep', None, 'tp'), may hold values from -0.125 to 0.125
- expert_down: bfloat16 [8, 1024, 2048], P('ep', 'tp'), may hold values from -0.1875 to 0.1875
- shared_gate: bfloat16 [2048, 512], P(None, 'tp'), may hold values from -0.125 to 0.125
- shared_up: bfloat16 [2048, 512], P(None, 'tp'), may hold values from -0.125 to 0.125
- shared_down: bfloat16 [512, 2048], P('tp'), may hold values from -0.25 to 0.25
Outputs:
- mixer_output: bfloat16 [4096, 2048], P(('ep', 'tp'))
- expert_output: bfloat16 [4096, 2048], P(('ep', 'tp'))
The draws below stay inside these ranges and needn't reach their ends.
Inputs may be any that keep to these rules, and one draw needn't show every extreme that they name: `expert_choice`: in each aligned block of 128 rows no expert is named by more than 64 rows, and in some block some expert is named by exactly 64 rows; the 2 entries of a row differ.
All inputs are finite; a program needn't handle non-finite values.
Results may differ from the reference program's by a relative error of at most 0.019.
Values may be sent and summed in bfloat16 or wider, within the bound.
A program may use at most 128 MiB of HBM per device.

```python
import math
import jax
import jax.numpy as jnp
import numpy as np
from jax import lax

D = 2048
HEADS = 24
KV_HEADS = 4
HEAD_DIM = 64
WINDOW = 128
SEQS = 1
EXPERT_FF = 1024
SHARED_FF = 512
TOP = 2
TOK_B_DEV = 128
EXPERTS = 8
TOKENS_A = 4096
TOKENS_B = 4096
SEQ_LEN = 4096
CAP = 64
N_TP = 4


def attention_weights(key):
    base_key = jax.random.fold_in(key, 41)
    key_part = jax.random.truncated_normal(jax.random.fold_in(base_key, 1), -4.0, 4.0, (D, KV_HEADS * HEAD_DIM), jnp.float32) * D ** (-0.5)
    query_part = jax.random.truncated_normal(jax.random.fold_in(base_key, 2), -4.0, 4.0, (D, HEADS * HEAD_DIM), jnp.float32) * D ** (-0.5)
    return (key_part, query_part)


def draw_key_weight(key, part):
    key_part, query_part = attention_weights(key)
    return key_part.astype(jnp.bfloat16)


def draw_query_weight(key, part):
    key_part, query_part = attention_weights(key)
    return query_part.astype(jnp.bfloat16)


def draw_mixer_input(key, part):
    base_key = jax.random.fold_in(key, 53)
    values = jax.random.truncated_normal(jax.random.fold_in(base_key, 1), -5.0, 5.0, (TOKENS_A, D), jnp.float32)
    return values.astype(jnp.bfloat16)


def steps_of(stream_key, dims, pieces, low, largest):
    def one(axis_at, parts):
        draws = jax.random.uniform(jax.random.fold_in(jax.random.fold_in(stream_key, 6), axis_at), (parts,), jnp.float32, low / len(pieces), largest / len(pieces))
        return jnp.repeat(jnp.exp(draws), dims[axis_at] // parts).reshape((-1,) + (1,) * (len(dims) - axis_at - 1))

    loudness = one(*pieces[0])
    for cut in pieces[1:]:
        loudness = loudness * one(*cut)
    return loudness


def deal_out(stream_key, own, number, rows, amount, top, most, lean):
    ranking = jax.random.permutation(stream_key, amount)
    crowded, ordinary = shares(amount, rows * top, most, lean, True), shares(amount, rows * top, most, lean, False)
    places = jnp.arange(amount)

    def named(tallies, turn):
        used = int((tallies > 0).sum())
        fixed = max(1, used // 4)
        moved = fixed + (places - fixed + turn * (used - fixed)) % max(1, amount - fixed)
        return jnp.zeros((amount,), jnp.int32).at[ranking[jnp.where(places < fixed, places, moved)]].set(jnp.asarray(tallies, jnp.int32))

    tallies = jnp.where(number % 4 == 0, named(crowded, number // 4), named(ordinary, number - number // 4 - 1))
    mixed = jax.random.permutation(jax.random.fold_in(own, 3), amount)
    source_of, sink = mixed[0:amount // 2 * 2:2], mixed[1:amount // 2 * 2:2]
    margin = jnp.minimum(tallies[source_of] - 1, most - tallies[sink]) // 2
    margin = jnp.where((source_of == ranking[0]) | (sink == ranking[0]) | (tallies[sink] == 0), 0, jnp.maximum(margin, 0))
    moved = jax.random.randint(jax.random.fold_in(own, 4), (amount // 2,), 0, 1 << 20) % (margin + 1)
    tallies = tallies.at[source_of].add(-moved).at[sink].add(moved)
    items = jnp.searchsorted(jnp.cumsum(tallies), jnp.arange(rows * top), side="right").astype(jnp.int32)
    listing = items.reshape(top, rows).T
    listing = listing[jax.random.permutation(jax.random.fold_in(own, 1), rows)]
    turn = jax.random.randint(jax.random.fold_in(own, 2), (rows, 1), 0, top)
    return jnp.take_along_axis(listing, (jnp.arange(top)[None, :] + turn) % top, axis=1)


def shares(number_of, total, bound, skew, full):
    loads = [(1 << 20) // math.isqrt(grade ** skew) + 1 for grade in range(1, number_of + 1)]
    largest = bound if full else min(bound, max(-(-total // number_of), total * loads[0] // sum(loads)))
    least = 1 if total - largest >= number_of - 1 else 0
    counts, surplus = [largest] + [least] * (number_of - 1), total - largest - least * (number_of - 1)
    while surplus > 0:
        movable = [i for i in range(1, number_of) if counts[i] < largest] or [i for i in range(1, number_of) if counts[i] < bound]
        whole, remaining = sum([loads[i] for i in movable]), surplus
        for i in movable:
            more = min(bound - counts[i], max(1, remaining * loads[i] // whole), surplus)
            counts[i] = counts[i] + more
            surplus = surplus - more
    return np.array(counts)


def bell_draw(own_key, dims, scale, bound, pieces=(), kind=jnp.bfloat16):
    entries = jax.random.normal(own_key, dims, jnp.float32) * scale
    if len(pieces) > 0:
        entries = steps_of(own_key, dims, pieces, -0.22, 0.18) * entries
    return jnp.clip(entries, min=-bound, max=bound).astype(kind)


def setup_inputs(seed: int = 0) -> dict:
    key_of = jax.random.split(jax.random.key(seed), 18)
    mixer_input = draw_mixer_input(jax.random.fold_in(key_of[17], 71), 0)
    expert_input = bell_draw(key_of[1], (TOKENS_B, D), 1.0, 6.0, ((0, 8),))
    gain_mixer = jnp.clip(1.0 + 0.18 * jax.random.normal(key_of[2], (D,), jnp.float32), 0.1, 1.9)
    gain_expert = jnp.clip(1.0 + 0.18 * jax.random.normal(key_of[3], (D,), jnp.float32), 0.1, 1.9)
    query_weight = draw_query_weight(jax.random.fold_in(key_of[17], 71), 0)
    key_weight = draw_key_weight(jax.random.fold_in(key_of[17], 71), 0)
    value_weight = bell_draw(key_of[6], (D, KV_HEADS * HEAD_DIM), D ** -0.5, 0.125, ((1, 4),))
    sink_logits = jnp.clip(2.0 + 4.0 * jax.random.uniform(key_of[7], (HEADS,), jnp.float32) ** steps_of(key_of[7], (HEADS,), ((0, 4),), -0.2, 0.2), 2.0, 6.0)
    output_weight = bell_draw(key_of[8], (HEADS * HEAD_DIM, D), (HEADS * HEAD_DIM // 25) ** -0.5, 0.75, ((0, 4),))
    expert_choice_keys = jax.random.split(jax.random.fold_in(key_of[9], 1), TOKENS_B // TOK_B_DEV)
    expert_choice_turns = jax.random.permutation(jax.random.fold_in(key_of[9], 3), TOKENS_B // TOK_B_DEV)
    expert_choice = jax.vmap(lambda own, number: deal_out(jax.random.fold_in(key_of[9], 2), own, number, TOK_B_DEV, EXPERTS, TOP, CAP, 2))(expert_choice_keys, expert_choice_turns).reshape((TOKENS_B, TOP))
    route_weights = jnp.clip(0.2 + 1 * jax.random.uniform(key_of[10], (TOKENS_B, TOP), jnp.float32) ** steps_of(key_of[10], (TOKENS_B, TOP), ((0, 8),), -0.2, 0.2), 0.2, 1.2)
    expert_gate = bell_draw(key_of[11], (EXPERTS, D, EXPERT_FF), D ** -0.5, 0.125, ((0, 8), (2, 4)))
    expert_up = bell_draw(key_of[12], (EXPERTS, D, EXPERT_FF), D ** -0.5, 0.125, ((0, 8), (2, 4)))
    expert_down = bell_draw(key_of[13], (EXPERTS, EXPERT_FF, D), EXPERT_FF ** -0.5, 0.1875, ((0, 8), (1, 4)))
    shared_gate = bell_draw(key_of[14], (D, SHARED_FF), D ** -0.5, 0.125, ((1, 4),))
    shared_up = bell_draw(key_of[15], (D, SHARED_FF), D ** -0.5, 0.125, ((1, 4),))
    shared_down = bell_draw(key_of[16], (SHARED_FF, D), SHARED_FF ** -0.5, 0.25, ((0, 4),))
    return dict(mixer_input=mixer_input, expert_input=expert_input, gain_mixer=gain_mixer, gain_expert=gain_expert, query_weight=query_weight, key_weight=key_weight, value_weight=value_weight, sink_logits=sink_logits, output_weight=output_weight, expert_choice=expert_choice, route_weights=route_weights, expert_gate=expert_gate, expert_up=expert_up, expert_down=expert_down, shared_gate=shared_gate, shared_up=shared_up, shared_down=shared_down)


norm_eps = 1e-06
rope_base = 500000.0

def rounded(value):
    return lax.optimization_barrier(value.astype(jnp.bfloat16)).astype(jnp.float32)

def rms_scale(matrix, scaling):
    widened = matrix.astype(jnp.float32)
    scaled = widened * lax.rsqrt(lax.optimization_barrier(jnp.mean(widened * widened, axis=-1, keepdims=True)) + norm_eps)
    return (scaled * scaling).astype(jnp.bfloat16)

def frequencies(head_size):
    half_steps = jnp.arange(head_size // 2, dtype=jnp.float32)
    return rope_base ** (-(2.0 * half_steps) / head_size)

def rotate(heads, angles):
    middle = heads.shape[-1] // 2
    widened = heads.astype(jnp.float32)
    cosine = jnp.cos(angles)[:, None, :]
    sine_val = jnp.sin(angles)[:, None, :]
    leading = widened[..., :middle]
    trailing = widened[..., middle:]
    turned = jnp.concatenate([leading * cosine - trailing * sine_val, trailing * cosine + leading * sine_val], axis=-1)
    return turned.astype(jnp.bfloat16)

def attend(query_heads, key_heads, value_heads, prior_keys, prior_values, first_position, sink_logits):
    window = prior_keys.shape[0]
    total_rows, kv_count, head_size = key_heads.shape
    group_size = query_heads.shape[1] // kv_count
    blocks = total_rows // window

    def banded(earlier, current):
        joined = jnp.concatenate([earlier, current], axis=0).reshape(blocks + 1, window, kv_count, head_size)
        return jnp.concatenate([joined[:-1], joined[1:]], axis=1)
    band_keys = banded(prior_keys, key_heads)
    band_values = banded(prior_values, value_heads)
    query_blocks = query_heads.reshape(blocks, window, kv_count, group_size, head_size)
    scores = jnp.einsum('nqhgd,nkhd->nhgqk', query_blocks.astype(jnp.float32), band_keys.astype(jnp.float32)) / math.sqrt(head_size)
    query_index = jnp.arange(window, dtype=jnp.int32)[:, None]
    key_index = jnp.arange(2 * window, dtype=jnp.int32)[None, :]
    distance = query_index + window - key_index
    block_start = first_position + jnp.arange(blocks, dtype=jnp.int32)[:, None, None] * window
    allowed = (distance >= 0) & (distance < window) & (block_start - window + key_index >= 0)
    scores = jnp.where(allowed[:, None, None, :, :], scores, -jnp.inf)
    sink_grid = sink_logits.astype(jnp.float32).reshape(kv_count, group_size)[None, :, :, None, None]
    row_peak = jnp.maximum(lax.optimization_barrier(jnp.max(scores, axis=-1, keepdims=True)), sink_grid)
    shifted_exp = jnp.exp(scores - row_peak)
    denominator = lax.optimization_barrier(jnp.sum(shifted_exp, axis=-1, keepdims=True)) + jnp.exp(sink_grid - row_peak)
    probs = (shifted_exp / denominator).astype(jnp.bfloat16)
    attended = jnp.einsum('nhgqk,nkhd->nqhgd', probs.astype(jnp.float32), band_values.astype(jnp.float32))
    return attended.astype(jnp.bfloat16).reshape(total_rows, kv_count * group_size * head_size)

def reference(mixer_input, expert_input, gain_mixer, gain_expert, query_weight, key_weight, value_weight, sink_logits, output_weight, expert_choice, route_weights, expert_gate, expert_up, expert_down, shared_gate, shared_up, shared_down):
    head_block = HEADS * HEAD_DIM // N_TP

    def one_sequence(seq_rows):
        normed = rms_scale(seq_rows, gain_mixer)
        queries = jnp.dot(normed, query_weight, preferred_element_type=jnp.float32).astype(jnp.bfloat16)
        key_rows = jnp.dot(normed, key_weight, preferred_element_type=jnp.float32).astype(jnp.bfloat16)
        value_rows = jnp.dot(normed, value_weight, preferred_element_type=jnp.float32).astype(jnp.bfloat16)
        positions = jnp.arange(SEQ_LEN, dtype=jnp.float32)
        angles = positions[:, None] * frequencies(HEAD_DIM)[None, :]
        rot_queries = rotate(queries.reshape(SEQ_LEN, HEADS, HEAD_DIM), angles)
        rot_keys = rotate(key_rows.reshape(SEQ_LEN, KV_HEADS, HEAD_DIM), angles)
        value_heads = value_rows.reshape(SEQ_LEN, KV_HEADS, HEAD_DIM)
        empty_rows = jnp.zeros((WINDOW, KV_HEADS, HEAD_DIM), jnp.bfloat16)
        attended = attend(rot_queries, rot_keys, value_heads, empty_rows, empty_rows, 0, sink_logits)
        mixed_sum = jnp.zeros((SEQ_LEN, D), jnp.float32)
        for slice_index in range(N_TP):
            low_edge = slice_index * head_block
            mixed_sum = mixed_sum + rounded(jnp.dot(attended[:, low_edge:low_edge + head_block], output_weight[low_edge:low_edge + head_block], preferred_element_type=jnp.float32))
        return mixed_sum.astype(jnp.bfloat16)
    mixer_output = lax.map(one_sequence, mixer_input.reshape(SEQS, SEQ_LEN, D)).reshape(TOKENS_A, D)
    normed_rows = rms_scale(expert_input, gain_expert)
    padded_rows = jnp.concatenate([normed_rows, jnp.zeros((1, D), jnp.bfloat16)], axis=0)
    block_count = TOKENS_B // TOK_B_DEV
    assigned = TOK_B_DEV * TOP
    picked_experts = expert_choice.reshape(block_count, assigned)
    onehot = (picked_experts[:, :, None] == jnp.arange(EXPERTS, dtype=jnp.int32)[None, None, :]).astype(jnp.int32)
    slot_ranks = lax.optimization_barrier(jnp.sum(jnp.cumsum(onehot, axis=1) * onehot, axis=-1)) - 1
    block_ids = jnp.arange(block_count, dtype=jnp.int32)[:, None]
    slot_index = (picked_experts * block_count + block_ids) * CAP + slot_ranks
    token_owner = block_ids * TOK_B_DEV + jnp.arange(assigned, dtype=jnp.int32)[None, :] // TOP
    slot_table = jnp.full((EXPERTS * block_count * CAP,), TOKENS_B, jnp.int32).at[slot_index.reshape(-1)].set(token_owner.reshape(-1).astype(jnp.int32))
    weight_table = jnp.zeros((EXPERTS * block_count * CAP,), jnp.float32).at[slot_index.reshape(-1)].set(route_weights.reshape(-1).astype(jnp.float32))
    ff_block = EXPERT_FF // N_TP

    def one_expert(carry, inputs):
        index_row, weight_row, gate_matrix, up_matrix, down_matrix = inputs
        chosen_rows = padded_rows[index_row]
        gate_values = jnp.dot(chosen_rows, gate_matrix, preferred_element_type=jnp.float32)
        up_values = jnp.dot(chosen_rows, up_matrix, preferred_element_type=jnp.float32)
        hidden = (jax.nn.silu(gate_values) * up_values).astype(jnp.bfloat16)
        result = jnp.zeros((chosen_rows.shape[0], D), jnp.float32)
        for slice_index in range(N_TP):
            low_edge = slice_index * ff_block
            result = result + rounded(jnp.dot(hidden[:, low_edge:low_edge + ff_block], down_matrix[low_edge:low_edge + ff_block], preferred_element_type=jnp.float32))
        return (carry.at[index_row].add(result * weight_row[:, None]), None)
    routed, unused = lax.scan(one_expert, jnp.zeros((TOKENS_B + 1, D), jnp.float32), (slot_table.reshape(EXPERTS, block_count * CAP), weight_table.reshape(EXPERTS, block_count * CAP), expert_gate, expert_up, expert_down))
    shared_gate_values = jnp.dot(normed_rows, shared_gate, preferred_element_type=jnp.float32)
    shared_up_values = jnp.dot(normed_rows, shared_up, preferred_element_type=jnp.float32)
    shared_hidden = (jax.nn.silu(shared_gate_values) * shared_up_values).astype(jnp.bfloat16)
    shared_block = SHARED_FF // N_TP
    shared_result = jnp.zeros((TOKENS_B, D), jnp.float32)
    for slice_index in range(N_TP):
        low_edge = slice_index * shared_block
        shared_result = shared_result + rounded(jnp.dot(shared_hidden[:, low_edge:low_edge + shared_block], shared_down[low_edge:low_edge + shared_block], preferred_element_type=jnp.float32))
    expert_output = (routed[:TOKENS_B] + shared_result).astype(jnp.bfloat16)
    return (mixer_output, expert_output)
```

```python
import functools
import math

import jax
import jax.numpy as jnp
from jax import lax
from jax.sharding import PartitionSpec as P

HEAD_DIM = 64
WINDOW = 128
SEQS = 1
CHUNKS = 2


norm_eps = 1e-06
rope_base = 500000.0


def from_behind(value, axis, steps):
    count = lax.axis_size(axis)
    first, last = (max(0, -steps), min(count, count - steps))
    return lax.ppermute(value, axis, [(source, source + steps) for source in range(first, last)])


def rounded(value):
    return lax.optimization_barrier(value.astype(jnp.bfloat16)).astype(jnp.float32)


def rms_scale(matrix, scaling):
    widened = matrix.astype(jnp.float32)
    scaled = widened * lax.rsqrt(jnp.mean(widened * widened, axis=-1, keepdims=True) + norm_eps)
    return (scaled * scaling).astype(jnp.bfloat16)


def frequencies(head_size):
    half_steps = jnp.arange(head_size // 2, dtype=jnp.float32)
    return rope_base ** (-(2.0 * half_steps) / head_size)


def rotate(heads, angles):
    middle = heads.shape[-1] // 2
    widened = heads.astype(jnp.float32)
    cosine = jnp.cos(angles)[:, None, :]
    sine_val = jnp.sin(angles)[:, None, :]
    leading = widened[..., :middle]
    trailing = widened[..., middle:]
    turned = jnp.concatenate(
        [leading * cosine - trailing * sine_val, trailing * cosine + leading * sine_val], axis=-1
    )
    return turned.astype(jnp.bfloat16)


def attend(
    query_heads, key_heads, value_heads, prior_keys, prior_values, first_position, sink_logits
):
    window = prior_keys.shape[0]
    total_rows, kv_count, head_size = key_heads.shape
    group_size = query_heads.shape[1] // kv_count
    blocks = total_rows // window

    def banded(earlier, current):
        joined = jnp.concatenate([earlier, current], axis=0).reshape(
            blocks + 1, window, kv_count, head_size
        )
        return jnp.concatenate([joined[:-1], joined[1:]], axis=1)

    band_keys = banded(prior_keys, key_heads)
    band_values = banded(prior_values, value_heads)
    query_blocks = query_heads.reshape(blocks, window, kv_count, group_size, head_size)
    scores = jnp.einsum(
        "nqhgd,nkhd->nhgqk", query_blocks, band_keys, preferred_element_type=jnp.float32
    ) / math.sqrt(head_size)
    query_index = jnp.arange(window, dtype=jnp.int32)[:, None]
    key_index = jnp.arange(2 * window, dtype=jnp.int32)[None, :]
    distance = query_index + window - key_index
    block_start = first_position + jnp.arange(blocks, dtype=jnp.int32)[:, None, None] * window
    allowed = (distance >= 0) & (distance < window) & (block_start - window + key_index >= 0)
    scores = jnp.where(allowed[:, None, None, :, :], scores, -jnp.inf)
    sink_grid = sink_logits.reshape(kv_count, group_size)[None, :, :, None, None]
    row_peak = jnp.maximum(jnp.max(scores, axis=-1, keepdims=True), sink_grid)
    shifted_exp = jnp.exp(scores - row_peak)
    denominator = jnp.sum(shifted_exp, axis=-1, keepdims=True) + jnp.exp(sink_grid - row_peak)
    probs = (shifted_exp / denominator).astype(jnp.bfloat16)
    attended = jnp.einsum(
        "nhgqk,nkhd->nqhgd", probs, band_values, preferred_element_type=jnp.float32
    )
    return attended.astype(jnp.bfloat16).reshape(total_rows, kv_count * group_size * head_size)


def sum_at_owner(value, axis):
    count = lax.axis_size(axis)
    if count & (count - 1):
        return lax.psum_scatter(value, axis, scatter_dimension=0, tiled=False)
    rank = lax.axis_index(axis)
    step = 1
    while step < count:
        paired = value.reshape(-1, 2, *value.shape[1:])
        side = rank // step % 2
        kept = lax.dynamic_index_in_dim(paired, side, 1, keepdims=False)
        sent = lax.dynamic_index_in_dim(paired, 1 - side, 1, keepdims=False)
        came = lax.ppermute(sent, axis, [(source, source ^ step) for source in range(count)])
        value = (kept.astype(jnp.float32) + came.astype(jnp.float32)).astype(jnp.bfloat16)
        step *= 2
    return value[0]


def local(
    mixer_input,
    expert_input,
    gain_mixer,
    gain_expert,
    query_weight,
    key_weight,
    value_weight,
    sink_logits,
    output_weight,
    expert_choice,
    route_weights,
    expert_gate,
    expert_up,
    expert_down,
    shared_gate,
    shared_up,
    shared_down,
):
    tp_count = lax.axis_size("tp")
    ep_count = lax.axis_size("ep")
    tp_rank = lax.axis_index("tp")
    group_rows, model_width = mixer_input.shape
    normed = rms_scale(mixer_input, gain_mixer)
    queries = jnp.dot(normed, query_weight, preferred_element_type=jnp.float32).astype(jnp.bfloat16)
    key_rows = jnp.dot(normed, key_weight, preferred_element_type=jnp.float32).astype(jnp.bfloat16)
    value_rows = jnp.dot(normed, value_weight, preferred_element_type=jnp.float32).astype(
        jnp.bfloat16
    )
    first_position = lax.axis_index("ep") % (ep_count // SEQS) * group_rows
    positions = (first_position + jnp.arange(group_rows, dtype=jnp.int32)).astype(jnp.float32)
    angles = positions[:, None] * frequencies(HEAD_DIM)[None, :]
    rot_queries = rotate(queries.reshape(group_rows, -1, HEAD_DIM), angles)
    rot_keys = rotate(key_rows.reshape(group_rows, -1, HEAD_DIM), angles)
    key_width = key_rows.shape[1]
    tail_start = group_rows - WINDOW
    tail_pair = jnp.concatenate(
        [rot_keys.reshape(group_rows, key_width)[tail_start:], value_rows[tail_start:]], axis=1
    )
    earlier_pair = from_behind(tail_pair, "ep", 1)
    prior_keys = earlier_pair[:, :key_width].reshape(WINDOW, -1, HEAD_DIM)
    prior_values = earlier_pair[:, key_width:].reshape(WINDOW, -1, HEAD_DIM)
    attended = attend(
        rot_queries,
        rot_keys,
        value_rows.reshape(group_rows, -1, HEAD_DIM),
        prior_keys,
        prior_values,
        first_position,
        sink_logits,
    )
    mixer_part = jnp.dot(attended, output_weight, preferred_element_type=jnp.float32).astype(
        jnp.bfloat16
    )
    group_tokens = expert_input.shape[0]
    own_tokens = group_tokens // tp_count
    top_count = expert_choice.shape[1]
    local_experts = expert_gate.shape[0]
    experts_all = local_experts * ep_count
    capacity = 2 * own_tokens * top_count // experts_all
    own_start = tp_rank * own_tokens
    own_choice = lax.dynamic_slice_in_dim(expert_choice, own_start, own_tokens, 0)
    own_weights = lax.dynamic_slice_in_dim(route_weights, own_start, own_tokens, 0)
    own_rows = rms_scale(
        lax.dynamic_slice_in_dim(expert_input, own_start, own_tokens, 0), gain_expert
    )
    expert_ids = jnp.arange(experts_all, dtype=jnp.int32)
    named = own_choice[:, :, None] == expert_ids[None, None, :]
    named_any = jnp.any(named, axis=1)
    token_ids = jnp.arange(own_tokens, dtype=jnp.int32)
    before = (token_ids[None, :] < token_ids[:, None]).astype(jnp.bfloat16)
    ranks = jnp.dot(
        before, named_any.astype(jnp.bfloat16), preferred_element_type=jnp.float32
    ).astype(jnp.int32)
    slot_of = own_choice * capacity + jnp.sum(jnp.where(named, ranks[:, None, :], 0), axis=-1)
    slot_ids = jnp.arange(experts_all * capacity, dtype=jnp.int32)
    picks = [slot_of[:, k, None] == slot_ids[None, :] for k in range(top_count)]
    spread = functools.reduce(jnp.logical_or, picks).astype(jnp.bfloat16)
    outgoing = (
        lax.dot_general(
            spread, own_rows, (((0,), (0,)), ((), ())), preferred_element_type=jnp.float32
        )
        .astype(jnp.bfloat16)
        .reshape(experts_all, capacity, model_width)
    )
    arrived = lax.all_gather(
        lax.all_to_all(outgoing, "ep", split_axis=0, concat_axis=0, tiled=True), "tp", axis=0
    )
    normed_rows = rms_scale(expert_input, gain_expert)
    gate_values = jnp.dot(normed_rows, shared_gate, preferred_element_type=jnp.float32)
    up_values = jnp.dot(normed_rows, shared_up, preferred_element_type=jnp.float32)
    hidden = (jax.nn.silu(gate_values) * up_values).astype(jnp.bfloat16)
    shared_part = jnp.dot(hidden, shared_down, preferred_element_type=jnp.float32).astype(
        jnp.bfloat16
    )
    arrived, mixer_part, shared_part = lax.optimization_barrier((arrived, mixer_part, shared_part))
    mixer_output = lax.psum_scatter(mixer_part, "tp", scatter_dimension=0, tiled=True)
    shared_own = lax.psum_scatter(shared_part, "tp", scatter_dimension=0, tiled=True)
    shaped = arrived.reshape(tp_count, ep_count, local_experts, capacity, model_width)
    gate_values = jnp.einsum(
        "jiecd,edf->jiecf", shaped, expert_gate, preferred_element_type=jnp.float32
    )
    up_values = jnp.einsum(
        "jiecd,edf->jiecf", shaped, expert_up, preferred_element_type=jnp.float32
    )
    hidden = (jax.nn.silu(gate_values) * up_values).astype(jnp.bfloat16)
    pieces = []
    width = model_width // CHUNKS
    for chunk in range(CHUNKS):
        partial = jnp.einsum(
            "jiecf,efd->jiecd",
            hidden,
            expert_down[:, :, chunk * width : (chunk + 1) * width],
            preferred_element_type=jnp.float32,
        ).astype(jnp.bfloat16)
        summed = sum_at_owner(partial.reshape(tp_count, -1, width), "tp")
        returned = lax.all_to_all(
            summed.reshape(experts_all, capacity, width),
            "ep",
            split_axis=0,
            concat_axis=0,
            tiled=True,
        ).reshape(-1, width)
        pieces.append(
            sum(
                jnp.dot(
                    picks[k].astype(jnp.bfloat16), returned, preferred_element_type=jnp.float32
                )
                * own_weights[:, k, None]
                for k in range(top_count)
            )
        )
    routed = jnp.concatenate(pieces, axis=1)
    expert_output = (routed + shared_own.astype(jnp.float32)).astype(jnp.bfloat16)
    return (mixer_output, expert_output)


def solution(mesh):
    placed = (
        P("ep", None),
        P("ep", None),
        P(),
        P(),
        P(None, "tp"),
        P(None, "tp"),
        P(None, "tp"),
        P("tp"),
        P("tp", None),
        P("ep", None),
        P("ep", None),
        P("ep", None, "tp"),
        P("ep", None, "tp"),
        P("ep", "tp", None),
        P(None, "tp"),
        P(None, "tp"),
        P("tp", None),
    )
    return jax.shard_map(
        local,
        mesh=mesh,
        in_specs=placed,
        out_specs=(P(("ep", "tp"), None), P(("ep", "tp"), None)),
        check_vma=False,
    )
```

```python
import functools
import math

import jax
import jax.numpy as jnp
from jax import lax
from jax.sharding import PartitionSpec as P

HEAD_DIM = 64
WINDOW = 128
SEQS = 1
CHUNKS = 2


norm_eps = 1e-06
rope_base = 500000.0


def from_behind(value, axis, steps):
    count = lax.axis_size(axis)
    first, last = (max(0, -steps), min(count, count - steps))
    return lax.ppermute(value, axis, [(source, source + steps) for source in range(first, last)])


def rounded(value):
    return lax.optimization_barrier(value.astype(jnp.bfloat16)).astype(jnp.float32)


def rms_scale(matrix, scaling):
    widened = matrix.astype(jnp.float32)
    scaled = widened * lax.rsqrt(jnp.mean(widened * widened, axis=-1, keepdims=True) + norm_eps)
    return (scaled * scaling).astype(jnp.bfloat16)


def frequencies(head_size):
    half_steps = jnp.arange(head_size // 2, dtype=jnp.float32)
    return rope_base ** (-(2.0 * half_steps) / head_size)


def rotate(heads, angles):
    middle = heads.shape[-1] // 2
    widened = heads.astype(jnp.float32)
    cosine = jnp.cos(angles)[:, None, :]
    sine_val = jnp.sin(angles)[:, None, :]
    leading = widened[..., :middle]
    trailing = widened[..., middle:]
    turned = jnp.concatenate(
        [leading * cosine - trailing * sine_val, trailing * cosine + leading * sine_val], axis=-1
    )
    return turned.astype(jnp.bfloat16)


def attend(
    query_heads, key_heads, value_heads, prior_keys, prior_values, first_position, sink_logits
):
    window = prior_keys.shape[0]
    total_rows, kv_count, head_size = key_heads.shape
    group_size = query_heads.shape[1] // kv_count
    blocks = total_rows // window

    def banded(earlier, current):
        joined = jnp.concatenate([earlier, current], axis=0).reshape(
            blocks + 1, window, kv_count, head_size
        )
        return jnp.concatenate([joined[:-1], joined[1:]], axis=1)

    band_keys = banded(prior_keys, key_heads)
    band_values = banded(prior_values, value_heads)
    query_blocks = query_heads.reshape(blocks, window, kv_count, group_size, head_size)
    scores = jnp.einsum(
        "nqhgd,nkhd->nhgqk", query_blocks, band_keys, preferred_element_type=jnp.float32
    ) / math.sqrt(head_size)
    query_index = jnp.arange(window, dtype=jnp.int32)[:, None]
    key_index = jnp.arange(2 * window, dtype=jnp.int32)[None, :]
    distance = query_index + window - key_index
    block_start = first_position + jnp.arange(blocks, dtype=jnp.int32)[:, None, None] * window
    allowed = (distance >= 0) & (distance < window) & (block_start - window + key_index >= 0)
    scores = jnp.where(allowed[:, None, None, :, :], scores, -jnp.inf)
    sink_grid = sink_logits.reshape(kv_count, group_size)[None, :, :, None, None]
    row_peak = jnp.maximum(jnp.max(scores, axis=-1, keepdims=True), sink_grid)
    shifted_exp = jnp.exp(scores - row_peak)
    denominator = jnp.sum(shifted_exp, axis=-1, keepdims=True) + jnp.exp(sink_grid - row_peak)
    probs = (shifted_exp / denominator).astype(jnp.bfloat16)
    attended = jnp.einsum(
        "nhgqk,nkhd->nqhgd", probs, band_values, preferred_element_type=jnp.float32
    )
    return attended.astype(jnp.bfloat16).reshape(total_rows, kv_count * group_size * head_size)


def sum_at_owner(value, axis):
    count = lax.axis_size(axis)
    if count & (count - 1):
        return lax.psum_scatter(value, axis, scatter_dimension=0, tiled=False)
    rank = lax.axis_index(axis)
    step = 1
    while step < count:
        paired = value.reshape(-1, 2, *value.shape[1:])
        side = rank // step % 2
        kept = lax.dynamic_index_in_dim(paired, side, 1, keepdims=False)
        sent = lax.dynamic_index_in_dim(paired, 1 - side, 1, keepdims=False)
        came = lax.ppermute(sent, axis, [(source, source ^ step) for source in range(count)])
        value = (kept.astype(jnp.float32) + came.astype(jnp.float32)).astype(jnp.bfloat16)
        step *= 2
    return value[0]


def local(
    mixer_input,
    expert_input,
    gain_mixer,
    gain_expert,
    query_weight,
    key_weight,
    value_weight,
    sink_logits,
    output_weight,
    expert_choice,
    route_weights,
    expert_gate,
    expert_up,
    expert_down,
    shared_gate,
    shared_up,
    shared_down,
):
    tp_count = lax.axis_size("tp")
    ep_count = lax.axis_size("ep")
    tp_rank = lax.axis_index("tp")
    group_rows, model_width = mixer_input.shape
    normed = rms_scale(mixer_input, gain_mixer)
    queries = jnp.dot(normed, query_weight, preferred_element_type=jnp.float32).astype(jnp.bfloat16)
    key_rows = jnp.dot(normed, key_weight, preferred_element_type=jnp.float32).astype(jnp.bfloat16)
    value_rows = jnp.dot(normed, value_weight, preferred_element_type=jnp.float32).astype(
        jnp.bfloat16
    )
    first_position = lax.axis_index("ep") % (ep_count // SEQS) * group_rows
    positions = (first_position + jnp.arange(group_rows, dtype=jnp.int32)).astype(jnp.float32)
    angles = positions[:, None] * frequencies(HEAD_DIM)[None, :]
    rot_queries = rotate(queries.reshape(group_rows, -1, HEAD_DIM), angles)
    rot_keys = rotate(key_rows.reshape(group_rows, -1, HEAD_DIM), angles)
    key_width = key_rows.shape[1]
    tail_start = group_rows - WINDOW
    tail_pair = jnp.concatenate(
        [rot_keys.reshape(group_rows, key_width)[tail_start:], value_rows[tail_start:]], axis=1
    )
    earlier_pair = from_behind(tail_pair, "ep", 1)
    prior_keys = earlier_pair[:, :key_width].reshape(WINDOW, -1, HEAD_DIM)
    prior_values = earlier_pair[:, key_width:].reshape(WINDOW, -1, HEAD_DIM)
    attended = attend(
        rot_queries,
        rot_keys,
        value_rows.reshape(group_rows, -1, HEAD_DIM),
        prior_keys,
        prior_values,
        first_position,
        sink_logits,
    )
    mixer_part = jnp.dot(attended, output_weight, preferred_element_type=jnp.float32).astype(
        jnp.bfloat16
    )
    group_tokens = expert_input.shape[0]
    own_tokens = group_tokens // tp_count
    top_count = expert_choice.shape[1]
    local_experts = expert_gate.shape[0]
    experts_all = local_experts * ep_count
    capacity = 2 * own_tokens * top_count // experts_all
    own_start = tp_rank * own_tokens
    own_choice = lax.dynamic_slice_in_dim(expert_choice, own_start, own_tokens, 0)
    own_weights = lax.dynamic_slice_in_dim(route_weights, own_start, own_tokens, 0)
    own_rows = rms_scale(
        lax.dynamic_slice_in_dim(expert_input, own_start, own_tokens, 0), gain_expert
    )
    expert_ids = jnp.arange(experts_all, dtype=jnp.int32)
    named = own_choice[:, :, None] == expert_ids[None, None, :]
    named_any = jnp.any(named, axis=1)
    token_ids = jnp.arange(own_tokens, dtype=jnp.int32)
    before = (token_ids[None, :] < token_ids[:, None]).astype(jnp.bfloat16)
    ranks = jnp.dot(
        before, named_any.astype(jnp.bfloat16), preferred_element_type=jnp.float32
    ).astype(jnp.int32)
    slot_of = own_choice * capacity + jnp.sum(jnp.where(named, ranks[:, None, :], 0), axis=-1)
    chunks = CHUNKS if capacity % CHUNKS == 0 else 1
    held = capacity // chunks
    flat_ids = jnp.arange(experts_all * held, dtype=jnp.int32)
    picks = []
    arrivals = []
    for chunk in range(chunks):
        slot_ids = flat_ids // held * capacity + chunk * held + flat_ids % held
        picked = [slot_of[:, k, None] == slot_ids[None, :] for k in range(top_count)]
        spread = functools.reduce(jnp.logical_or, picked).astype(jnp.bfloat16)
        outgoing = (
            lax.dot_general(
                spread, own_rows, (((0,), (0,)), ((), ())), preferred_element_type=jnp.float32
            )
            .astype(jnp.bfloat16)
            .reshape(experts_all, held, model_width)
        )
        arrivals.append(
            lax.all_gather(
                lax.all_to_all(outgoing, "ep", split_axis=0, concat_axis=0, tiled=True),
                "tp",
                axis=0,
            )
        )
        picks.append(picked)
    normed_rows = rms_scale(expert_input, gain_expert)
    gate_values = jnp.dot(normed_rows, shared_gate, preferred_element_type=jnp.float32)
    up_values = jnp.dot(normed_rows, shared_up, preferred_element_type=jnp.float32)
    hidden = (jax.nn.silu(gate_values) * up_values).astype(jnp.bfloat16)
    shared_part = jnp.dot(hidden, shared_down, preferred_element_type=jnp.float32).astype(
        jnp.bfloat16
    )
    arrivals[-1], mixer_part, shared_part = lax.optimization_barrier(
        (arrivals[-1], mixer_part, shared_part)
    )
    mixer_output = lax.psum_scatter(mixer_part, "tp", scatter_dimension=0, tiled=True)
    shared_own = lax.psum_scatter(shared_part, "tp", scatter_dimension=0, tiled=True)
    routed = 0.0
    for arrived, picked in zip(arrivals, picks):
        shaped = arrived.reshape(tp_count, ep_count, local_experts, held, model_width)
        gate_values = jnp.einsum(
            "jiecd,edf->jiecf", shaped, expert_gate, preferred_element_type=jnp.float32
        )
        up_values = jnp.einsum(
            "jiecd,edf->jiecf", shaped, expert_up, preferred_element_type=jnp.float32
        )
        hidden = (jax.nn.silu(gate_values) * up_values).astype(jnp.bfloat16)
        partial = jnp.einsum(
            "jiecf,efd->jiecd", hidden, expert_down, preferred_element_type=jnp.float32
        ).astype(jnp.bfloat16)
        summed = sum_at_owner(partial.reshape(tp_count, -1, model_width), "tp")
        returned = lax.all_to_all(
            summed.reshape(experts_all, held, model_width),
            "ep",
            split_axis=0,
            concat_axis=0,
            tiled=True,
        ).reshape(-1, model_width)
        for k in range(top_count):
            routed = routed + own_weights[:, k, None] * jnp.dot(
                picked[k].astype(jnp.bfloat16), returned, preferred_element_type=jnp.float32
            )
    expert_output = (routed + shared_own.astype(jnp.float32)).astype(jnp.bfloat16)
    return (mixer_output, expert_output)


def solution(mesh):
    placed = (
        P("ep", None),
        P("ep", None),
        P(),
        P(),
        P(None, "tp"),
        P(None, "tp"),
        P(None, "tp"),
        P("tp"),
        P("tp", None),
        P("ep", None),
        P("ep", None),
        P("ep", None, "tp"),
        P("ep", None, "tp"),
        P("ep", "tp", None),
        P(None, "tp"),
        P(None, "tp"),
        P("tp", None),
    )
    return jax.shard_map(
        local,
        mesh=mesh,
        in_specs=placed,
        out_specs=(P(("ep", "tp"), None), P(("ep", "tp"), None)),
        check_vma=False,
    )
```
